32 devices in a mesh: sp: 16 (over z, y, x), tp: 2 (over core).
Axes of the slice: x: 2, y: 2, z: 4, core: 2. Of those that a mesh axis runs over, the one named last changes fastest.
Arguments:
- query_matrix: bfloat16 [4096, 2048], P('sp', 'tp'), may hold values from -6 to 6
- key_matrix: bfloat16 [4096, 2048], P('sp', 'tp'), may hold values from -6 to 6
- value_matrix: bfloat16 [4096, 2048], P('sp', 'tp'), may hold values from -6 to 6
- output_gate_logits: bfloat16 [4096, 2048], P('sp', 'tp'), may hold values from -6 to 6
- decay_preactivation: bfloat16 [4096, 2048], P('sp', 'tp'), may hold values from -3 to 12
- head_extra_decay: float32 [4096, 32], P('sp', 'tp'), may hold values from -0.7 to 0
- residual: bfloat16 [4096, 2048], P(('sp', 'tp')), may hold values from -6 to 6
- head_norm_gain: float32 [64], replicated, may hold values from 0.1 to 1.9
- output_projection_weight: bfloat16 [2048, 2048], P('tp'), may hold values from -0.125 to 0.125
- mixer_norm_gain: float32 [2048], replicated, may hold values from 0.1 to 1.9
- routes: int32 [4096, 2], P(('sp', 'tp')), may hold values from 0 to 15, all different within a row; in each aligned block of 128 rows (0 to 127, 128 to 255, ...) at most 32 rows name the same one
- routing_weight: float32 [4096, 2], P(('sp', 'tp')), may hold values from 0.2 to 1.5
- routed_gate_weight: bfloat16 [16, 2048, 1024], P('sp', None, 'tp'), may hold values from -0.125 to 0.125
- routed_up_weight: bfloat16 [16, 2048, 1024], P('sp', None, 'tp'), may hold values from -0.125 to 0.125
- routed_down_weight: bfloat16 [16, 1024, 2048], P('sp', 'tp'), may hold values from -0.1875 to 0.1875
- common_gate_weight: bfloat16 [2048, 512], replicated, may hold values from -0.125 to 0.125
- common_up_weight: bfloat16 [2048, 512], replicated, may hold values from -0.125 to 0.125
- common_down_weight: bfloat16 [512, 2048], replicated, may hold values from -0.25 to 0.25
- final_norm_gain: float32 [2048], replicated, may hold values from 0.1 to 1.9
Outputs:
- layer_out: bfloat16 [4096, 2048], P(('sp', 'tp'))
The draws below stay inside these ranges and needn't reach their ends.
Inputs may be any that keep to these rules, and one draw needn't show every extreme that they name: `routes`: each row names 2 different experts. In the rows of one device (aligned blocks of rows) no expert is named by more than 32 rows, a bound that some block reaches.
All inputs are finite; a program needn't handle non-finite values.
Results may differ from the reference program's by a relative error of at most 0.019.
Values may be sent and summed in bfloat16 or wider, within the bound.
A program may use at most 192 MiB of HBM per device.

```python
import math
import jax
import jax.numpy as jnp
import numpy as np
from jax import lax

D = 2048
HEAD_NUMBER = 32
KEY_HEAD_SIZE = 64
BLOCK_TOKENS = 64
FE = 1024
FS = 512
TOP_K = 2
TOK_DEV = 256
SEQUENCE_TOKENS = 4096
EXPERTS = 16
CAP = 32
N_SP = 16
N_TP = 2


def draw_decay_preactivation(key, part):
    head_key, fast_key, slow_key, device_key, noise_key = jax.random.split(key, 5)
    fast_share = 0.5
    fast_head = jax.random.uniform(head_key, (HEAD_NUMBER,), jnp.float32) < fast_share
    fast_level = jax.random.uniform(fast_key, (HEAD_NUMBER, KEY_HEAD_SIZE), jnp.float32, -0.5, 1.0)
    slow_level = math.log(SEQUENCE_TOKENS / 9.6) + jax.random.uniform(slow_key, (HEAD_NUMBER, KEY_HEAD_SIZE), jnp.float32, -0.7, 0.7)
    level = jnp.where(fast_head[:, None], fast_level, slow_level).reshape(1, HEAD_NUMBER * KEY_HEAD_SIZE)
    device_shift = jax.random.uniform(device_key, (SEQUENCE_TOKENS // TOK_DEV, 1), jnp.float32, -0.7, 0.7)
    device_shift = jnp.repeat(device_shift, TOK_DEV, axis=0, total_repeat_length=SEQUENCE_TOKENS)
    noise = 0.7 * jax.random.normal(noise_key, (SEQUENCE_TOKENS, HEAD_NUMBER * KEY_HEAD_SIZE), jnp.float32)
    return jnp.clip(level + device_shift + noise, -3.0, 12.0).astype(jnp.bfloat16)


def draw_head_extra_decay(key, part):
    place_key, dropout_random_key = jax.random.split(key)
    places = jax.random.randint(place_key, (8,), 0, SEQUENCE_TOKENS)
    removed_entries = jnp.any(jnp.arange(SEQUENCE_TOKENS)[:, None] == places[None, :], axis=1)
    spike_dropped = jax.random.uniform(dropout_random_key, (SEQUENCE_TOKENS, HEAD_NUMBER), jnp.float32, -0.7, -0.22)
    return jnp.where(removed_entries[:, None], spike_dropped, 0.0).astype(jnp.float32)


def steps_of(key, dims, pieces, least, top_value):
    factor_of = 1.0
    for position, shards_of in pieces:
        heights = jax.random.uniform(jax.random.fold_in(jax.random.fold_in(key, 6), position), (shards_of,), jnp.float32, least / len(pieces), top_value / len(pieces))
        factor_of = factor_of * jnp.repeat(jnp.exp(heights), dims[position] // shards_of).reshape((-1,) + (1,) * (len(dims) - 1 - position))
    return factor_of


def shared_out(key, own, number, rows, amount, top, most, lean):
    sequence = jax.random.permutation(key, amount)
    heavy_load, common = shares(amount, rows * top, most, lean, True), shares(amount, rows * top, most, lean, False)
    places = jnp.arange(amount)

    def named(lengths, turn):
        used = int((lengths > 0).sum())
        fixed = max(1, used // 4)
        shifted = fixed + (places - fixed + turn * (used - fixed)) % max(1, amount - fixed)
        return jnp.zeros((amount,), jnp.int32).at[sequence[jnp.where(places < fixed, places, shifted)]].set(jnp.asarray(lengths, jnp.int32))

    lengths = jnp.where(number % 4 == 0, named(heavy_load, number // 4), named(common, number - number // 4 - 1))
    mixed = jax.random.permutation(jax.random.fold_in(own, 3), amount)
    donor, receiver = mixed[0:amount // 2 * 2:2], mixed[1:amount // 2 * 2:2]
    room = jnp.minimum(lengths[donor] - 1, most - lengths[receiver]) // 2
    room = jnp.where((donor == sequence[0]) | (receiver == sequence[0]) | (lengths[receiver] == 0), 0, jnp.maximum(room, 0))
    shifted = jax.random.randint(jax.random.fold_in(own, 4), (amount // 2,), 0, 1 << 20) % (room + 1)
    lengths = lengths.at[donor].add(-shifted).at[receiver].add(shifted)
    labels = jnp.searchsorted(jnp.cumsum(lengths), jnp.arange(rows * top), side="right").astype(jnp.int32)
    grid = labels.reshape(top, rows).T
    grid = grid[jax.random.permutation(jax.random.fold_in(own, 1), rows)]
    turn = jax.random.randint(jax.random.fold_in(own, 2), (rows, 1), 0, top)
    return jnp.take_along_axis(grid, (jnp.arange(top)[None, :] + turn) % top, axis=1)


def shares(amount, total, bound, lean, full):
    portions = [(1 << 20) // math.isqrt(rank ** lean) + 1 for rank in range(1, amount + 1)]
    largest = bound if full else min(bound, max(-(-total // amount), total * portions[0] // sum(portions)))
    least = 1 if total - largest >= amount - 1 else 0
    given, spare = [largest] + [least] * (amount - 1), total - largest - least * (amount - 1)
    while spare > 0:
        free = [i for i in range(1, amount) if given[i] < largest] or [i for i in range(1, amount) if given[i] < bound]
        whole, budget = sum([portions[i] for i in free]), spare
        for i in free:
            addition = min(bound - given[i], max(1, budget * portions[i] // whole), spare)
            given[i] = given[i] + addition
            spare = spare - addition
    return np.array(given)


def bell_draw(stream_key, dims, width, bound, cuts=(), kind=jnp.bfloat16):
    entries = width * jax.random.normal(stream_key, dims, jnp.float32)
    if cuts:
        entries = entries * steps_of(stream_key, dims, cuts, -0.22, 0.18)
    return jnp.clip(entries, -bound, bound).astype(kind)


def setup_inputs(seed: int = 0) -> dict:
    streams_of = jax.random.split(jax.random.key(seed), 20)
    query_matrix = bell_draw(streams_of[0], (SEQUENCE_TOKENS, HEAD_NUMBER * KEY_HEAD_SIZE), 1.0, 6.0, ((0, 16), (1, 2)))
    key_matrix = bell_draw(streams_of[1], (SEQUENCE_TOKENS, HEAD_NUMBER * KEY_HEAD_SIZE), 1.0, 6.0, ((0, 16), (1, 2)))
    value_matrix = bell_draw(streams_of[2], (SEQUENCE_TOKENS, HEAD_NUMBER * KEY_HEAD_SIZE), 1.0, 6.0, ((0, 16), (1, 2)))
    output_gate_logits = bell_draw(streams_of[3], (SEQUENCE_TOKENS, HEAD_NUMBER * KEY_HEAD_SIZE), 1.0, 6.0, ((0, 16), (1, 2)))
    decay_preactivation = draw_decay_preactivation(jax.random.fold_in(streams_of[19], 71), 0)
    head_extra_decay = draw_head_extra_decay(jax.random.fold_in(streams_of[19], 71), 0)
    residual = bell_draw(streams_of[6], (SEQUENCE_TOKENS, D), 1.0, 6.0, ((0, 32),))
    head_norm_gain = jnp.clip(1.0 + 0.18 * jax.random.normal(streams_of[7], (KEY_HEAD_SIZE,), jnp.float32), 0.1, 1.9)
    output_projection_weight = bell_draw(streams_of[8], (HEAD_NUMBER * KEY_HEAD_SIZE, D), (HEAD_NUMBER * KEY_HEAD_SIZE) ** -0.5, 0.125, ((0, 2),))
    mixer_norm_gain = jnp.clip(1.0 + 0.18 * jax.random.normal(streams_of[9], (D,), jnp.float32), 0.1, 1.9)
    routes_keys = jax.random.split(jax.random.fold_in(streams_of[10], 1), SEQUENCE_TOKENS // (TOK_DEV // N_TP))
    routes_turns = jax.random.permutation(jax.random.fold_in(streams_of[10], 3), SEQUENCE_TOKENS // (TOK_DEV // N_TP))
    routes = jax.vmap(lambda own, number: shared_out(jax.random.fold_in(streams_of[10], 2), own, number, TOK_DEV // N_TP, EXPERTS, TOP_K, CAP, 1))(routes_keys, routes_turns).reshape((SEQUENCE_TOKENS, TOP_K))
    routing_weight = jnp.clip(0.2 + 1.3 * jax.random.uniform(streams_of[11], (SEQUENCE_TOKENS, TOP_K), jnp.float32) ** steps_of(streams_of[11], (SEQUENCE_TOKENS, TOP_K), ((0, 32),), -0.2, 0.2), 0.2, 1.5)
    routed_gate_weight = bell_draw(streams_of[12], (EXPERTS, D, FE), D ** -0.5, 0.125, ((0, 16), (2, 2)))
    routed_up_weight = bell_draw(streams_of[13], (EXPERTS, D, FE), D ** -0.5, 0.125, ((0, 16), (2, 2)))
    routed_down_weight = bell_draw(streams_of[14], (EXPERTS, FE, D), FE ** -0.5, 0.1875, ((0, 16), (1, 2)))
    common_gate_weight = bell_draw(streams_of[15], (D, FS), D ** -0.5, 0.125)
    common_up_weight = bell_draw(streams_of[16], (D, FS), D ** -0.5, 0.125)
    common_down_weight = bell_draw(streams_of[17], (FS, D), FS ** -0.5, 0.25)
    final_norm_gain = jnp.clip(1.0 + 0.18 * jax.random.normal(streams_of[18], (D,), jnp.float32), 0.1, 1.9)
    return {"query_matrix": query_matrix, "key_matrix": key_matrix, "value_matrix": value_matrix, "output_gate_logits": output_gate_logits, "decay_preactivation": decay_preactivation, "head_extra_decay": head_extra_decay, "residual": residual, "head_norm_gain": head_norm_gain, "output_projection_weight": output_projection_weight, "mixer_norm_gain": mixer_norm_gain, "routes": routes, "routing_weight": routing_weight, "routed_gate_weight": routed_gate_weight, "routed_up_weight": routed_up_weight, "routed_down_weight": routed_down_weight, "common_gate_weight": common_gate_weight, "common_up_weight": common_up_weight, "common_down_weight": common_down_weight, "final_norm_gain": final_norm_gain}


EPS = 1e-06
GATE_DIVISOR = 16.0

def round_half(values):
    return lax.optimization_barrier(values.astype(jnp.bfloat16)).astype(jnp.float32)

def layer_norm(values, gain):
    center = values - lax.optimization_barrier(jnp.mean(values, axis=-1, keepdims=True))
    spread = lax.optimization_barrier(jnp.mean(center * center, axis=-1, keepdims=True))
    return center * lax.rsqrt(spread + EPS) * gain

def prepare_inputs(blocked_queries, blocked_keys, blocked_decay, spike_block_decay):
    logarithm_decay = jax.nn.log_sigmoid(blocked_decay.astype(jnp.float32)).reshape(BLOCK_TOKENS, HEAD_NUMBER, KEY_HEAD_SIZE) / GATE_DIVISOR
    logarithm_decay = logarithm_decay + spike_block_decay[:, :, None]
    inside_block = jnp.cumsum(logarithm_decay, axis=0)
    query_float = blocked_queries.astype(jnp.float32).reshape(BLOCK_TOKENS, HEAD_NUMBER, KEY_HEAD_SIZE) * KEY_HEAD_SIZE ** (-0.5)
    key_float = blocked_keys.astype(jnp.float32).reshape(BLOCK_TOKENS, HEAD_NUMBER, KEY_HEAD_SIZE)
    return (inside_block, query_float, key_float)

def forward_block(left_state, fragments):
    blocked_queries, blocked_keys, blocked_values, blocked_decay, spike_block_decay = fragments
    inside_block, query_float, key_float = prepare_inputs(blocked_queries, blocked_keys, blocked_decay, spike_block_decay)
    value_f = blocked_values.astype(jnp.float32).reshape(BLOCK_TOKENS, HEAD_NUMBER, KEY_HEAD_SIZE)
    total = inside_block[-1]
    query_up = query_float * jnp.exp(inside_block)
    query_down = query_float * jnp.exp(-inside_block)
    key_up = key_float * jnp.exp(inside_block)
    key_down = key_float * jnp.exp(-inside_block)
    lower_mask = jnp.tril(jnp.ones((BLOCK_TOKENS, BLOCK_TOKENS), bool))
    ahead = jnp.einsum('ihc,jhc->hij', query_up, key_down)
    behind = jnp.einsum('ihc,jhc->hij', query_down, key_up)
    scores = jnp.where(lower_mask, ahead, 0.0) + jnp.where(lower_mask, 0.0, behind)
    block_out = jnp.einsum('hij,jhv->ihv', scores, value_f)
    block_out = block_out + jnp.einsum('ihc,hcv->ihv', query_up, left_state)
    key_end = key_float * jnp.exp(total[None] - inside_block)
    new_state = jnp.exp(total)[..., None] * left_state + jnp.einsum('jhc,jhv->hcv', key_end, value_f)
    return (new_state, block_out)

def backward_block(right_state, fragments):
    blocked_queries, blocked_keys, blocked_values, blocked_decay, spike_block_decay = fragments
    inside_block, query_float, key_float = prepare_inputs(blocked_queries, blocked_keys, blocked_decay, spike_block_decay)
    value_f = blocked_values.astype(jnp.float32).reshape(BLOCK_TOKENS, HEAD_NUMBER, KEY_HEAD_SIZE)
    total = inside_block[-1]
    query_tail = query_float * jnp.exp(total[None] - inside_block)
    block_out = jnp.einsum('ihc,hcv->ihv', query_tail, right_state)
    key_up = key_float * jnp.exp(inside_block)
    new_state = jnp.exp(total)[..., None] * right_state + jnp.einsum('jhc,jhv->hcv', key_up, value_f)
    return (new_state, block_out)

def reference(query_matrix, key_matrix, value_matrix, output_gate_logits, decay_preactivation, head_extra_decay, residual, head_norm_gain, output_projection_weight, mixer_norm_gain, routes, routing_weight, routed_gate_weight, routed_up_weight, routed_down_weight, common_gate_weight, common_up_weight, common_down_weight, final_norm_gain):
    token_count = query_matrix.shape[0]
    number_of_blocks = token_count // BLOCK_TOKENS
    fragments = (query_matrix.reshape(number_of_blocks, BLOCK_TOKENS, HEAD_NUMBER * KEY_HEAD_SIZE), key_matrix.reshape(number_of_blocks, BLOCK_TOKENS, HEAD_NUMBER * KEY_HEAD_SIZE), value_matrix.reshape(number_of_blocks, BLOCK_TOKENS, HEAD_NUMBER * KEY_HEAD_SIZE), decay_preactivation.reshape(number_of_blocks, BLOCK_TOKENS, HEAD_NUMBER * KEY_HEAD_SIZE), head_extra_decay.reshape(number_of_blocks, BLOCK_TOKENS, HEAD_NUMBER))
    zero_state = jnp.zeros((HEAD_NUMBER, KEY_HEAD_SIZE, KEY_HEAD_SIZE), jnp.float32)
    _, forward_out = lax.scan(forward_block, zero_state, fragments)
    _, backward_out = lax.scan(backward_block, zero_state, fragments, reverse=True)
    mixed = (forward_out + backward_out).reshape(token_count, HEAD_NUMBER, KEY_HEAD_SIZE)
    normed_heads = mixed * lax.rsqrt(lax.optimization_barrier(jnp.mean(mixed * mixed, axis=-1, keepdims=True)) + EPS) * head_norm_gain
    gated = (normed_heads.reshape(token_count, HEAD_NUMBER * KEY_HEAD_SIZE) * jax.nn.silu(output_gate_logits.astype(jnp.float32))).astype(jnp.bfloat16)
    group_width = HEAD_NUMBER * KEY_HEAD_SIZE // N_TP
    projected = jnp.zeros((token_count, D), jnp.float32)
    for group in range(N_TP):
        part_sum = jnp.dot(gated[:, group * group_width:(group + 1) * group_width], output_projection_weight[group * group_width:(group + 1) * group_width], preferred_element_type=jnp.float32)
        projected = projected + round_half(part_sum)
    normed = layer_norm(residual.astype(jnp.float32) + projected, mixer_norm_gain).astype(jnp.bfloat16)
    sources = N_SP * N_TP
    row_count = TOK_DEV // N_TP
    assigned = row_count * TOP_K
    flat_routes = routes.reshape(sources, assigned)
    member = (flat_routes[:, :, None] == jnp.arange(EXPERTS, dtype=jnp.int32)[None, None, :]).astype(jnp.int32)
    rank_in = lax.optimization_barrier(jnp.sum((jnp.cumsum(member, axis=1) - member) * member, axis=2))
    column = jnp.arange(sources, dtype=jnp.int32)[:, None] * CAP + rank_in
    token_index = jnp.arange(sources, dtype=jnp.int32)[:, None] * row_count + jnp.arange(assigned, dtype=jnp.int32)[None, :] // TOP_K
    token_table = jnp.zeros((EXPERTS, sources * CAP), jnp.int32).at[flat_routes, column].set(token_index)
    weight_table = jnp.zeros((EXPERTS, sources * CAP), jnp.float32).at[flat_routes, column].set(routing_weight.reshape(sources, assigned))
    half_width = FE // N_TP

    def per_expert(total, expert_pieces):
        tokens_here, weights_here, gate_here, up_here, down_here = expert_pieces
        picked = normed[tokens_here]
        gate_part = jnp.dot(picked, gate_here, preferred_element_type=jnp.float32)
        up_part = jnp.dot(picked, up_here, preferred_element_type=jnp.float32)
        inner = (jax.nn.silu(gate_part) * up_part).astype(jnp.bfloat16)
        expert_sum = jnp.zeros((picked.shape[0], D), jnp.float32)
        for group in range(N_TP):
            expert_sum = expert_sum + round_half(jnp.dot(inner[:, group * half_width:(group + 1) * half_width], down_here[group * half_width:(group + 1) * half_width], preferred_element_type=jnp.float32))
        expert_result = round_half(expert_sum)
        return (total.at[tokens_here].add(weights_here[:, None] * expert_result), None)
    routed, _ = lax.scan(per_expert, jnp.zeros((token_count, D), jnp.float32), (token_table, weight_table, routed_gate_weight, routed_up_weight, routed_down_weight))
    shared_gate_out = jnp.dot(normed, common_gate_weight, preferred_element_type=jnp.float32)
    shared_up_out = jnp.dot(normed, common_up_weight, preferred_element_type=jnp.float32)
    shared_inner = (jax.nn.silu(shared_gate_out) * shared_up_out).astype(jnp.bfloat16)
    feed = jnp.dot(shared_inner, common_down_weight, preferred_element_type=jnp.float32) + routed
    return layer_norm(normed.astype(jnp.float32) + feed, final_norm_gain).astype(jnp.bfloat16)
```

```python
import functools

import jax
import jax.numpy as jnp
from jax import lax
from jax.experimental import pallas as pl
from jax.experimental.pallas import tpu as pltpu
from jax.sharding import PartitionSpec as P

KEY_HEAD_SIZE = 64
BLOCK_TOKENS = 64


EPS = 1e-06
GATE_DIVISOR = 16.0


def layer_norm(values, gain):
    center = values - jnp.mean(values, axis=-1, keepdims=True)
    spread = jnp.mean(center * center, axis=-1, keepdims=True)
    return center * lax.rsqrt(spread + EPS) * gain


LANES = 128
MESH = pl.DeviceIdType.MESH


def lane_half(rows):
    return lax.broadcasted_iota(jnp.int32, (rows, LANES), 1) < KEY_HEAD_SIZE


def local_kernel(q_ref, k_ref, v_ref, decay_ref, extra_ref, out_ref, wide_ref, state_ref, total_ref):
    pair = pl.program_id(0)
    tokens = q_ref.shape[0]
    heads = extra_ref.shape[1]
    block = BLOCK_TOKENS
    half = lane_half(tokens)
    decay = decay_ref[...].astype(jnp.float32)
    logarithm = jnp.minimum(decay, 0.0) - jnp.log1p(jnp.exp(-jnp.abs(decay)))
    row = lax.broadcasted_iota(jnp.int32, (heads, LANES), 0)
    lane = lax.broadcasted_iota(jnp.int32, (heads, LANES), 1)
    chosen = (row == pair * (LANES // KEY_HEAD_SIZE) + lane // KEY_HEAD_SIZE).astype(jnp.float32)
    extra = jnp.dot(
        extra_ref[...], chosen, precision=lax.Precision.HIGHEST, preferred_element_type=jnp.float32
    )
    logarithm = logarithm * (1.0 / GATE_DIVISOR) + extra
    at = lax.broadcasted_iota(jnp.int32, (tokens, tokens), 0)
    other = lax.broadcasted_iota(jnp.int32, (tokens, tokens), 1)
    summed = jnp.dot(
        (other <= at).astype(jnp.float32),
        logarithm,
        precision=lax.Precision.HIGHEST,
        preferred_element_type=jnp.float32,
    )
    total = summed[tokens - 1 : tokens]
    query = q_ref[...].astype(jnp.float32) * KEY_HEAD_SIZE ** (-0.5)
    key = k_ref[...].astype(jnp.float32)
    value = v_ref[...]
    grown, rest = jnp.exp(summed), jnp.exp(total - summed)
    wide_ref[:, :LANES] = (query * grown).astype(jnp.bfloat16)
    wide_ref[:, LANES:] = (query * rest).astype(jnp.bfloat16)
    over = (((0,), (0,)), ((), ()))
    left = lax.dot_general(
        (key * rest).astype(jnp.bfloat16), value, over, preferred_element_type=jnp.float32
    )
    right = lax.dot_general(
        (key * grown).astype(jnp.bfloat16), value, over, preferred_element_type=jnp.float32
    )
    few = lane_half(KEY_HEAD_SIZE)
    top, low = slice(0, KEY_HEAD_SIZE), slice(KEY_HEAD_SIZE, LANES)
    first = jnp.where(few, left[top], pltpu.roll(right[top], KEY_HEAD_SIZE, 1))
    second = jnp.where(few, pltpu.roll(left[low], KEY_HEAD_SIZE, 1), right[low])
    state_ref[top] = first.astype(jnp.bfloat16)
    state_ref[low] = second.astype(jnp.bfloat16)
    total_ref[0] = total
    apart = (((1,), (1,)), ((), ()))
    small = lane_half(block)
    for place in range(tokens // block):
        begin, end = place * block, (place + 1) * block
        own = summed[begin:end]
        before = summed[begin - 1 : begin] if place else jnp.zeros((1, LANES), jnp.float32)
        after = summed[end - 1 : end]
        mine = query[begin:end]
        ups = mine * jnp.exp(own - before)
        tails = mine * jnp.exp(after - own)
        ups = jnp.concatenate([jnp.where(small, ups, 0.0), jnp.where(small, 0.0, ups)], axis=0)
        tails = jnp.concatenate(
            [jnp.where(small, tails, 0.0), jnp.where(small, 0.0, tails)], axis=0
        )
        key_left = key * jnp.exp(jnp.minimum(before - summed, 64.0))
        key_right = key * jnp.exp(jnp.minimum(summed - after, 64.0))
        ahead = lax.dot_general(
            ups.astype(jnp.bfloat16),
            key_left.astype(jnp.bfloat16),
            apart,
            preferred_element_type=jnp.float32,
        )
        behind = lax.dot_general(
            tails.astype(jnp.bfloat16),
            key_right.astype(jnp.bfloat16),
            apart,
            preferred_element_type=jnp.float32,
        )
        here = lax.broadcasted_iota(jnp.int32, (2 * block, tokens), 0)
        here = jnp.where(here < block, here, here - block) + begin
        there = lax.broadcasted_iota(jnp.int32, (2 * block, tokens), 1)
        scores = jnp.where(there <= here, ahead, behind).astype(jnp.bfloat16)
        both = jnp.dot(scores, value, preferred_element_type=jnp.float32)
        out_ref[begin:end] = jnp.where(small, both[:block], both[block:])


def local_part(query, key, value, decay, extra):
    tokens, width = query.shape
    pairs = width // LANES
    column = pl.BlockSpec((tokens, LANES), lambda p: (0, p))
    return pl.pallas_call(
        local_kernel,
        grid=(pairs,),
        in_specs=[column] * 4 + [pl.BlockSpec(extra.shape, lambda p: (0, 0))],
        out_specs=[
            column,
            pl.BlockSpec((tokens, 2 * LANES), lambda p: (0, p)),
            pl.BlockSpec((LANES, LANES), lambda p: (p, 0)),
            pl.BlockSpec((1, 1, LANES), lambda p: (p, 0, 0)),
        ],
        out_shape=[
            jax.ShapeDtypeStruct((tokens, width), jnp.float32),
            jax.ShapeDtypeStruct((tokens, 2 * width), jnp.bfloat16),
            jax.ShapeDtypeStruct((width, LANES), jnp.bfloat16),
            jax.ShapeDtypeStruct((pairs, 1, LANES), jnp.float32),
        ],
        name="local_part",
    )(query, key, value, decay, extra)


def exchange_kernel(
    n,
    state_ref,
    total_ref,
    out_ref,
    arrived,
    totals,
    ordered,
    before,
    outbound,
    send_state,
    recv_state,
    send_total,
    recv_total,
    send_back,
    recv_back,
):
    me = lax.axis_index("sp")
    rows = state_ref.shape[0] // n
    barrier = pltpu.get_barrier_semaphore()

    def greet(off, c):
        pl.semaphore_signal(
            barrier, inc=1, device_id={"sp": lax.rem(me + off, n)}, device_id_type=MESH
        )
        return c

    lax.fori_loop(1, n, greet, 0)
    pl.semaphore_wait(barrier, n - 1)

    def forth(off):
        to = lax.rem(me + off, n)
        first = pltpu.make_async_remote_copy(
            src_ref=state_ref.at[pl.ds(pl.multiple_of(to * rows, rows), rows)],
            dst_ref=arrived.at[off],
            send_sem=send_state.at[off],
            recv_sem=recv_state.at[off],
            device_id={"sp": to},
            device_id_type=MESH,
        )
        second = pltpu.make_async_remote_copy(
            src_ref=total_ref,
            dst_ref=totals.at[off],
            send_sem=send_total.at[off],
            recv_sem=recv_total.at[off],
            device_id={"sp": to},
            device_id_type=MESH,
        )
        return first, second

    def back(off):
        to = lax.rem(me + off, n)
        return pltpu.make_async_remote_copy(
            src_ref=outbound.at[to],
            dst_ref=out_ref.at[pl.ds(pl.multiple_of(me * rows, rows), rows)],
            send_sem=send_back.at[off],
            recv_sem=recv_back.at[off],
            device_id={"sp": to},
            device_id_type=MESH,
        )

    def start_forth(off, c):
        for copy in forth(off):
            copy.start()
        return c

    def wait_forth(off, c):
        for copy in forth(off):
            copy.wait()
        return c

    def start_back(off, c):
        back(off).start()
        return c

    def wait_back(off, c):
        back(off).wait()
        return c

    lax.fori_loop(1, n, start_forth, 0)
    mine = pl.ds(pl.multiple_of(me * rows, rows), rows)
    arrived[0] = state_ref[mine]
    totals[0] = total_ref[...]
    ordered[...] = jnp.zeros_like(ordered)
    lax.fori_loop(1, n, wait_forth, 0)
    group, shift = me * rows // LANES, lax.rem(me * rows, LANES)
    for k in range(n):
        ordered[k : k + 1] = totals[lax.rem(me - k + n, n), group]
    turned = pltpu.roll(ordered[...], lax.rem(LANES - shift, LANES), 1)
    weights = jnp.exp(turned.T)[:rows]
    half = lane_half(rows)
    carried = jnp.zeros((rows, LANES), jnp.float32)
    for k in range(n):
        before[k] = carried
        if k < n - 1:
            carried = weights[:, k : k + 1] * carried + arrived[lax.rem(me - k + n, n)].astype(
                jnp.float32
            )
    carried = jnp.zeros((rows, LANES), jnp.float32)
    for k in range(n - 1, -1, -1):
        outbound[k] = jnp.where(half, before[k], carried).astype(jnp.bfloat16)
        if k:
            carried = weights[:, k : k + 1] * carried + arrived[lax.rem(me - k + n, n)].astype(
                jnp.float32
            )
    lax.fori_loop(1, n, start_back, 0)
    out_ref[mine] = outbound[me]
    lax.fori_loop(1, n, wait_back, 0)


def exchange(state, total):
    n = lax.axis_size("sp")
    rows = state.shape[0] // n
    dma = pltpu.SemaphoreType.DMA((n,))
    return pl.pallas_call(
        functools.partial(exchange_kernel, n),
        in_specs=[pl.BlockSpec(memory_space=pltpu.VMEM)] * 2,
        out_specs=pl.BlockSpec(memory_space=pltpu.VMEM),
        out_shape=jax.ShapeDtypeStruct(state.shape, state.dtype),
        scratch_shapes=[
            pltpu.VMEM((n, rows, LANES), state.dtype),
            pltpu.VMEM((n,) + total.shape, jnp.float32),
            pltpu.VMEM((LANES, LANES), jnp.float32),
            pltpu.VMEM((n, rows, LANES), jnp.float32),
            pltpu.VMEM((n, rows, LANES), state.dtype),
            dma,
            dma,
            dma,
            dma,
            dma,
            dma,
        ],
        compiler_params=pltpu.CompilerParams(collective_id=0, has_side_effects=True),
        name="exchange",
    )(state, total)


def finish_kernel(local_ref, wide_ref, state_ref, logits_ref, gain_ref, out_ref):
    few = lane_half(KEY_HEAD_SIZE)
    first = state_ref[:KEY_HEAD_SIZE].astype(jnp.float32)
    second = state_ref[KEY_HEAD_SIZE:].astype(jnp.float32)
    states = jnp.concatenate(
        [
            jnp.where(few, first, 0.0),
            jnp.where(few, 0.0, pltpu.roll(second, KEY_HEAD_SIZE, 1)),
            jnp.where(few, pltpu.roll(first, KEY_HEAD_SIZE, 1), 0.0),
            jnp.where(few, 0.0, second),
        ],
        axis=0,
    ).astype(jnp.bfloat16)
    mixed = local_ref[...] + jnp.dot(wide_ref[...], states, preferred_element_type=jnp.float32)
    half = lane_half(mixed.shape[0])
    squares = mixed * mixed
    one = jnp.sum(jnp.where(half, squares, 0.0), axis=1, keepdims=True)
    two = jnp.sum(jnp.where(half, 0.0, squares), axis=1, keepdims=True)
    scale = jnp.where(
        half, lax.rsqrt(one / KEY_HEAD_SIZE + EPS), lax.rsqrt(two / KEY_HEAD_SIZE + EPS)
    )
    gate = jax.nn.silu(logits_ref[...].astype(jnp.float32))
    out_ref[...] = (mixed * scale * gain_ref[...] * gate).astype(jnp.bfloat16)


def finish_part(local, wide, state, logits, gain):
    tokens, width = local.shape
    column = pl.BlockSpec((tokens, LANES), lambda p: (0, p))
    return pl.pallas_call(
        finish_kernel,
        grid=(width // LANES,),
        in_specs=[
            column,
            pl.BlockSpec((tokens, 2 * LANES), lambda p: (0, p)),
            pl.BlockSpec((LANES, LANES), lambda p: (p, 0)),
            column,
            pl.BlockSpec((1, LANES), lambda p: (0, 0)),
        ],
        out_specs=column,
        out_shape=jax.ShapeDtypeStruct((tokens, width), jnp.bfloat16),
        name="finish_part",
    )(local, wide, state, logits, gain)


def expert_half(arrived, gate_half, up_half, down_half):
    flat_rows = arrived.reshape(-1, arrived.shape[-1])
    gate_part = jnp.dot(flat_rows, gate_half, preferred_element_type=jnp.float32)
    up_part = jnp.dot(flat_rows, up_half, preferred_element_type=jnp.float32)
    inner = (jax.nn.silu(gate_part) * up_part).astype(jnp.bfloat16)
    partial_out = jnp.dot(inner, down_half, preferred_element_type=jnp.float32).astype(jnp.bfloat16)
    return partial_out.reshape(arrived.shape)


def per_device(
    query_matrix,
    key_matrix,
    value_matrix,
    output_gate_logits,
    decay_preactivation,
    head_extra_decay,
    residual,
    head_norm_gain,
    output_projection_weight,
    mixer_norm_gain,
    routes,
    routing_weight,
    routed_gate_weight,
    routed_up_weight,
    routed_down_weight,
    common_gate_weight,
    common_up_weight,
    common_down_weight,
    final_norm_gain,
):
    local_out, wide, state, total = local_part(
        query_matrix, key_matrix, value_matrix, decay_preactivation, head_extra_decay
    )
    entered = exchange(state, total)
    gain = jnp.concatenate([head_norm_gain] * (LANES // KEY_HEAD_SIZE))[None]
    gated = finish_part(local_out, wide, entered, output_gate_logits, gain)
    projected = lax.psum_scatter(
        jnp.dot(gated, output_projection_weight, preferred_element_type=jnp.float32).astype(
            jnp.bfloat16
        ),
        "tp",
        scatter_dimension=0,
        tiled=True,
    ).astype(jnp.float32)
    normed = layer_norm(residual.astype(jnp.float32) + projected, mixer_norm_gain).astype(
        jnp.bfloat16
    )
    row_count = normed.shape[0]
    model_width = normed.shape[1]
    top_count = routes.shape[1]
    experts = lax.axis_size("sp")
    capacity = max(2, row_count * top_count // experts * 2)
    flat_expert = routes.reshape(-1)
    member = (flat_expert[:, None] == jnp.arange(experts, dtype=jnp.int32)[None, :]).astype(
        jnp.int32
    )
    rank_in = jnp.sum((jnp.cumsum(member, axis=0) - member) * member, axis=1)
    slot_of = flat_expert * capacity + rank_in
    source_row = (
        jnp.zeros((experts * capacity,), jnp.int32)
        .at[slot_of]
        .set(jnp.arange(row_count * top_count, dtype=jnp.int32) // top_count)
    )
    outbound = normed[source_row].reshape(experts, capacity, model_width)
    gate_half = routed_gate_weight[0]
    up_half = routed_up_weight[0]
    down_half = routed_down_weight[0]
    paired = lax.all_gather(
        lax.all_to_all(outbound, "sp", split_axis=0, concat_axis=0, tiled=True),
        "tp",
        axis=0,
        tiled=True,
    )
    partial_out = expert_half(paired, gate_half, up_half, down_half).astype(jnp.float32)
    summed = lax.psum_scatter(
        partial_out.astype(jnp.bfloat16), "tp", scatter_dimension=0, tiled=True
    )
    expert_out = lax.all_to_all(summed, "sp", split_axis=0, concat_axis=0, tiled=True)
    flat_out = expert_out.reshape(experts * capacity, model_width)
    picked = flat_out[slot_of].astype(jnp.float32).reshape(row_count, top_count, model_width)
    routed = jnp.einsum("rk,rkd->rd", routing_weight, picked)
    shared_gate_out = jnp.dot(normed, common_gate_weight, preferred_element_type=jnp.float32)
    shared_up_out = jnp.dot(normed, common_up_weight, preferred_element_type=jnp.float32)
    shared_inner = (jax.nn.silu(shared_gate_out) * shared_up_out).astype(jnp.bfloat16)
    feed = jnp.dot(shared_inner, common_down_weight, preferred_element_type=jnp.float32) + routed
    return layer_norm(normed.astype(jnp.float32) + feed, final_norm_gain).astype(jnp.bfloat16)


def solution(mesh):
    placed = (
        P("sp", "tp"),
        P("sp", "tp"),
        P("sp", "tp"),
        P("sp", "tp"),
        P("sp", "tp"),
        P("sp", "tp"),
        P(("sp", "tp"), None),
        P(),
        P("tp", None),
        P(),
        P(("sp", "tp"), None),
        P(("sp", "tp"), None),
        P("sp", None, "tp"),
        P("sp", None, "tp"),
        P("sp", "tp", None),
        P(),
        P(),
        P(),
        P(),
    )
    return jax.shard_map(
        per_device, mesh=mesh, in_specs=placed, out_specs=P(("sp", "tp"), None), check_vma=False
    )
```

```python
import functools

import jax
import jax.numpy as jnp
from jax import lax
from jax.experimental import pallas as pl
from jax.experimental.pallas import tpu as pltpu
from jax.sharding import PartitionSpec as P

KEY_HEAD_SIZE = 64
BLOCK_TOKENS = 64


EPS = 1e-06
GATE_DIVISOR = 16.0


def layer_norm(values, gain):
    center = values - jnp.mean(values, axis=-1, keepdims=True)
    spread = jnp.mean(center * center, axis=-1, keepdims=True)
    return center * lax.rsqrt(spread + EPS) * gain


LANES = 128
MESH = pl.DeviceIdType.MESH


def lane_half(rows):
    return lax.broadcasted_iota(jnp.int32, (rows, LANES), 1) < KEY_HEAD_SIZE


def local_kernel(q_ref, k_ref, v_ref, decay_ref, extra_ref, out_ref, wide_ref, state_ref, total_ref):
    pair = pl.program_id(0)
    tokens = q_ref.shape[0]
    heads = extra_ref.shape[1]
    block = BLOCK_TOKENS
    half = lane_half(tokens)
    decay = decay_ref[...].astype(jnp.float32)
    logarithm = jnp.minimum(decay, 0.0) - jnp.log1p(jnp.exp(-jnp.abs(decay)))
    row = lax.broadcasted_iota(jnp.int32, (heads, LANES), 0)
    lane = lax.broadcasted_iota(jnp.int32, (heads, LANES), 1)
    chosen = (row == pair * (LANES // KEY_HEAD_SIZE) + lane // KEY_HEAD_SIZE).astype(jnp.float32)
    extra = jnp.dot(
        extra_ref[...], chosen, precision=lax.Precision.HIGHEST, preferred_element_type=jnp.float32
    )
    logarithm = logarithm * (1.0 / GATE_DIVISOR) + extra
    at = lax.broadcasted_iota(jnp.int32, (tokens, tokens), 0)
    other = lax.broadcasted_iota(jnp.int32, (tokens, tokens), 1)
    summed = jnp.dot(
        (other <= at).astype(jnp.float32),
        logarithm,
        precision=lax.Precision.HIGHEST,
        preferred_element_type=jnp.float32,
    )
    total = summed[tokens - 1 : tokens]
    query = q_ref[...].astype(jnp.float32) * KEY_HEAD_SIZE ** (-0.5)
    key = k_ref[...].astype(jnp.float32)
    value = v_ref[...]
    grown, rest = jnp.exp(summed), jnp.exp(total - summed)
    wide_ref[:, :LANES] = (query * grown).astype(jnp.bfloat16)
    wide_ref[:, LANES:] = (query * rest).astype(jnp.bfloat16)
    over = (((0,), (0,)), ((), ()))
    left = lax.dot_general(
        (key * rest).astype(jnp.bfloat16), value, over, preferred_element_type=jnp.float32
    )
    right = lax.dot_general(
        (key * grown).astype(jnp.bfloat16), value, over, preferred_element_type=jnp.float32
    )
    few = lane_half(KEY_HEAD_SIZE)
    top, low = slice(0, KEY_HEAD_SIZE), slice(KEY_HEAD_SIZE, LANES)
    first = jnp.where(few, left[top], pltpu.roll(right[top], KEY_HEAD_SIZE, 1))
    second = jnp.where(few, pltpu.roll(left[low], KEY_HEAD_SIZE, 1), right[low])
    state_ref[top] = first.astype(jnp.bfloat16)
    state_ref[low] = second.astype(jnp.bfloat16)
    total_ref[0] = total
    apart = (((1,), (1,)), ((), ()))
    small = lane_half(block)
    for place in range(tokens // block):
        begin, end = place * block, (place + 1) * block
        own = summed[begin:end]
        before = summed[begin - 1 : begin] if place else jnp.zeros((1, LANES), jnp.float32)
        after = summed[end - 1 : end]
        mine = query[begin:end]
        ups = mine * jnp.exp(own - before)
        tails = mine * jnp.exp(after - own)
        ups = jnp.concatenate([jnp.where(small, ups, 0.0), jnp.where(small, 0.0, ups)], axis=0)
        tails = jnp.concatenate(
            [jnp.where(small, tails, 0.0), jnp.where(small, 0.0, tails)], axis=0
        )
        key_left = key * jnp.exp(jnp.minimum(before - summed, 64.0))
        key_right = key * jnp.exp(jnp.minimum(summed - after, 64.0))
        ahead = lax.dot_general(
            ups.astype(jnp.bfloat16),
            key_left.astype(jnp.bfloat16),
            apart,
            preferred_element_type=jnp.float32,
        )
        behind = lax.dot_general(
            tails.astype(jnp.bfloat16),
            key_right.astype(jnp.bfloat16),
            apart,
            preferred_element_type=jnp.float32,
        )
        here = lax.broadcasted_iota(jnp.int32, (2 * block, tokens), 0)
        here = jnp.where(here < block, here, here - block) + begin
        there = lax.broadcasted_iota(jnp.int32, (2 * block, tokens), 1)
        scores = jnp.where(there <= here, ahead, behind).astype(jnp.bfloat16)
        both = jnp.dot(scores, value, preferred_element_type=jnp.float32)
        out_ref[begin:end] = jnp.where(small, both[:block], both[block:])


def local_part(query, key, value, decay, extra):
    tokens, width = query.shape
    pairs = width // LANES
    column = pl.BlockSpec((tokens, LANES), lambda p: (0, p))
    return pl.pallas_call(
        local_kernel,
        grid=(pairs,),
        in_specs=[column] * 4 + [pl.BlockSpec(extra.shape, lambda p: (0, 0))],
        out_specs=[
            column,
            pl.BlockSpec((tokens, 2 * LANES), lambda p: (0, p)),
            pl.BlockSpec((LANES, LANES), lambda p: (p, 0)),
            pl.BlockSpec((1, 1, LANES), lambda p: (p, 0, 0)),
        ],
        out_shape=[
            jax.ShapeDtypeStruct((tokens, width), jnp.float32),
            jax.ShapeDtypeStruct((tokens, 2 * width), jnp.bfloat16),
            jax.ShapeDtypeStruct((width, LANES), jnp.bfloat16),
            jax.ShapeDtypeStruct((pairs, 1, LANES), jnp.float32),
        ],
        name="local_part",
    )(query, key, value, decay, extra)


def exchange_kernel(
    n,
    state_ref,
    total_ref,
    out_ref,
    arrived,
    totals,
    ordered,
    before,
    outbound,
    send_state,
    recv_state,
    send_total,
    recv_total,
    send_back,
    recv_back,
):
    me = lax.axis_index("sp")
    rows = state_ref.shape[0] // n
    barrier = pltpu.get_barrier_semaphore()

    def greet(off, c):
        pl.semaphore_signal(
            barrier, inc=1, device_id={"sp": lax.rem(me + off, n)}, device_id_type=MESH
        )
        return c

    lax.fori_loop(1, n, greet, 0)
    pl.semaphore_wait(barrier, n - 1)

    def forth(off):
        to = lax.rem(me + off, n)
        first = pltpu.make_async_remote_copy(
            src_ref=state_ref.at[pl.ds(pl.multiple_of(to * rows, rows), rows)],
            dst_ref=arrived.at[off],
            send_sem=send_state.at[off],
            recv_sem=recv_state.at[off],
            device_id={"sp": to},
            device_id_type=MESH,
        )
        second = pltpu.make_async_remote_copy(
            src_ref=total_ref,
            dst_ref=totals.at[off],
            send_sem=send_total.at[off],
            recv_sem=recv_total.at[off],
            device_id={"sp": to},
            device_id_type=MESH,
        )
        return first, second

    def back(off):
        to = lax.rem(me + off, n)
        return pltpu.make_async_remote_copy(
            src_ref=outbound.at[to],
            dst_ref=out_ref.at[pl.ds(pl.multiple_of(me * rows, rows), rows)],
            send_sem=send_back.at[off],
            recv_sem=recv_back.at[off],
            device_id={"sp": to},
            device_id_type=MESH,
        )

    def start_forth(off, c):
        for copy in forth(off):
            copy.start()
        return c

    def wait_forth(off, c):
        for copy in forth(off):
            copy.wait()
        return c

    def start_back(off, c):
        back(off).start()
        return c

    def wait_back(off, c):
        back(off).wait()
        return c

    lax.fori_loop(1, n, start_forth, 0)
    mine = pl.ds(pl.multiple_of(me * rows, rows), rows)
    arrived[0] = state_ref[mine]
    totals[0] = total_ref[...]
    ordered[...] = jnp.zeros_like(ordered)
    lax.fori_loop(1, n, wait_forth, 0)
    group, shift = me * rows // LANES, lax.rem(me * rows, LANES)
    for k in range(n):
        ordered[k : k + 1] = totals[lax.rem(me - k + n, n), group]
    turned = pltpu.roll(ordered[...], lax.rem(LANES - shift, LANES), 1)
    weights = jnp.exp(turned.T)[:rows]
    half = lane_half(rows)
    carried = jnp.zeros((rows, LANES), jnp.float32)
    for k in range(n):
        before[k] = carried
        if k < n - 1:
            carried = weights[:, k : k + 1] * carried + arrived[lax.rem(me - k + n, n)].astype(
                jnp.float32
            )
    carried = jnp.zeros((rows, LANES), jnp.float32)
    for k in range(n - 1, -1, -1):
        outbound[k] = jnp.where(half, before[k], carried).astype(jnp.bfloat16)
        if k:
            carried = weights[:, k : k + 1] * carried + arrived[lax.rem(me - k + n, n)].astype(
                jnp.float32
            )
    lax.fori_loop(1, n, start_back, 0)
    out_ref[mine] = outbound[me]
    lax.fori_loop(1, n, wait_back, 0)


def exchange(state, total):
    n = lax.axis_size("sp")
    rows = state.shape[0] // n
    dma = pltpu.SemaphoreType.DMA((n,))
    return pl.pallas_call(
        functools.partial(exchange_kernel, n),
        in_specs=[pl.BlockSpec(memory_space=pltpu.VMEM)] * 2,
        out_specs=pl.BlockSpec(memory_space=pltpu.VMEM),
        out_shape=jax.ShapeDtypeStruct(state.shape, state.dtype),
        scratch_shapes=[
            pltpu.VMEM((n, rows, LANES), state.dtype),
            pltpu.VMEM((n,) + total.shape, jnp.float32),
            pltpu.VMEM((LANES, LANES), jnp.float32),
            pltpu.VMEM((n, rows, LANES), jnp.float32),
            pltpu.VMEM((n, rows, LANES), state.dtype),
            dma,
            dma,
            dma,
            dma,
            dma,
            dma,
        ],
        compiler_params=pltpu.CompilerParams(collective_id=0, has_side_effects=True),
        name="exchange",
    )(state, total)


def finish_kernel(local_ref, wide_ref, state_ref, logits_ref, gain_ref, out_ref):
    few = lane_half(KEY_HEAD_SIZE)
    first = state_ref[:KEY_HEAD_SIZE].astype(jnp.float32)
    second = state_ref[KEY_HEAD_SIZE:].astype(jnp.float32)
    states = jnp.concatenate(
        [
            jnp.where(few, first, 0.0),
            jnp.where(few, 0.0, pltpu.roll(second, KEY_HEAD_SIZE, 1)),
            jnp.where(few, pltpu.roll(first, KEY_HEAD_SIZE, 1), 0.0),
            jnp.where(few, 0.0, second),
        ],
        axis=0,
    ).astype(jnp.bfloat16)
    mixed = local_ref[...] + jnp.dot(wide_ref[...], states, preferred_element_type=jnp.float32)
    half = lane_half(mixed.shape[0])
    squares = mixed * mixed
    one = jnp.sum(jnp.where(half, squares, 0.0), axis=1, keepdims=True)
    two = jnp.sum(jnp.where(half, 0.0, squares), axis=1, keepdims=True)
    scale = jnp.where(
        half, lax.rsqrt(one / KEY_HEAD_SIZE + EPS), lax.rsqrt(two / KEY_HEAD_SIZE + EPS)
    )
    gate = jax.nn.silu(logits_ref[...].astype(jnp.float32))
    out_ref[...] = (mixed * scale * gain_ref[...] * gate).astype(jnp.bfloat16)


def finish_part(local, wide, state, logits, gain):
    tokens, width = local.shape
    column = pl.BlockSpec((tokens, LANES), lambda p: (0, p))
    return pl.pallas_call(
        finish_kernel,
        grid=(width // LANES,),
        in_specs=[
            column,
            pl.BlockSpec((tokens, 2 * LANES), lambda p: (0, p)),
            pl.BlockSpec((LANES, LANES), lambda p: (p, 0)),
            column,
            pl.BlockSpec((1, LANES), lambda p: (0, 0)),
        ],
        out_specs=column,
        out_shape=jax.ShapeDtypeStruct((tokens, width), jnp.bfloat16),
        name="finish_part",
    )(local, wide, state, logits, gain)


GROUP = 4


def expert_kernel(
    n,
    sent_ref,
    gate_hbm,
    up_hbm,
    down_hbm,
    result_ref,
    rows_in,
    gate_ref,
    up_ref,
    down_ref,
    kept,
    given,
    taken,
    summed,
    send_out,
    recv_out,
    send_row,
    recv_row,
    send_part,
    recv_part,
    send_back,
    recv_back,
    local,
):
    me, core = lax.axis_index("sp"), lax.axis_index("tp")
    groups = n // GROUP
    capacity, width = sent_ref.shape[1:]
    peer = {"tp": 1 - core}

    def target(off):
        high = lax.rem(me // GROUP + off // GROUP, groups)
        return high * GROUP + lax.rem(lax.rem(me, GROUP) + lax.rem(off, GROUP), GROUP)

    def origin(off):
        high = lax.rem(me // GROUP - off // GROUP + groups, groups)
        return high * GROUP + lax.rem(lax.rem(me, GROUP) - lax.rem(off, GROUP) + GROUP, GROUP)

    def remote(source, destination, send, recv, device):
        return pltpu.make_async_remote_copy(
            src_ref=source,
            dst_ref=destination,
            send_sem=send,
            recv_sem=recv,
            device_id=device,
            device_id_type=MESH,
        )

    def outward(off):
        return remote(
            sent_ref.at[target(off)],
            rows_in.at[off // GROUP, 0, lax.rem(off, GROUP)],
            send_out.at[off],
            recv_out.at[off],
            {"sp": target(off)},
        )

    def homeward(off):
        return remote(
            summed.at[off // GROUP, lax.rem(off, GROUP)],
            result_ref.at[me],
            send_back.at[off],
            recv_back.at[off],
            {"sp": origin(off)},
        )

    loads = [
        pltpu.make_async_copy(gate_hbm, gate_ref, local.at[0]),
        pltpu.make_async_copy(up_hbm, up_ref, local.at[1]),
        pltpu.make_async_copy(down_hbm, down_ref, local.at[2]),
        pltpu.make_async_copy(sent_ref.at[me], rows_in.at[0, 0, 0], local.at[3]),
    ]
    for load in loads:
        load.start()
    barrier = pltpu.get_barrier_semaphore()

    def greet(off, c):
        pl.semaphore_signal(barrier, inc=1, device_id={"sp": target(off)}, device_id_type=MESH)
        return c

    lax.fori_loop(1, n, greet, 0)
    pl.semaphore_signal(barrier, inc=1, device_id=peer, device_id_type=MESH)
    pl.semaphore_wait(barrier, n)

    def start_outward(off, c):
        outward(off).start()
        return c

    lax.fori_loop(1, n, start_outward, 0)
    for load in loads:
        load.wait()

    def arrive(off, c):
        outward(off).wait_recv()
        return c

    def start_homeward(off, c):
        homeward(off).start()
        return c

    def step(group, c):
        begin = group * GROUP
        skip = 1 - (group + groups - 1) // groups
        lax.fori_loop(begin + skip, begin + GROUP, arrive, 0)
        share = remote(
            rows_in.at[group, 0],
            rows_in.at[group, 1],
            send_row.at[group],
            recv_row.at[group],
            peer,
        )
        share.start()
        share.wait()
        rows = rows_in[group].reshape(2 * GROUP * capacity, width)
        gate = jnp.dot(rows, gate_ref[...], preferred_element_type=jnp.float32)
        up = jnp.dot(rows, up_ref[...], preferred_element_type=jnp.float32)
        inner = (jax.nn.silu(gate) * up).astype(jnp.bfloat16)
        part = jnp.dot(inner, down_ref[...], preferred_element_type=jnp.float32)
        part = part.astype(jnp.bfloat16).reshape(2, GROUP, capacity, width)
        given[group] = part[1]
        kept[...] = part[0]
        trade = remote(
            given.at[group], taken.at[group], send_part.at[group], recv_part.at[group], peer
        )
        trade.start()
        trade.wait()
        summed[group] = (
            kept[...].astype(jnp.float32) + taken[group].astype(jnp.float32)
        ).astype(jnp.bfloat16)
        lax.fori_loop(begin + skip, begin + GROUP, start_homeward, 0)
        return c

    lax.fori_loop(0, groups, step, 0)
    result_ref[me] = summed[0, 0]

    def finish(off, c):
        outward(off).wait_send()
        homeward(off).wait()
        return c

    lax.fori_loop(1, n, finish, 0)


def expert_exchange(sent, gate_half, up_half, down_half):
    n, capacity, width = sent.shape
    groups = n // GROUP
    block = (groups, GROUP, capacity, width)
    each, few = pltpu.SemaphoreType.DMA((n,)), pltpu.SemaphoreType.DMA((groups,))
    vmem, anywhere = pl.BlockSpec(memory_space=pltpu.VMEM), pl.BlockSpec(memory_space=pl.ANY)
    return pl.pallas_call(
        functools.partial(expert_kernel, n),
        in_specs=[vmem] + [anywhere] * 3,
        out_specs=vmem,
        out_shape=jax.ShapeDtypeStruct(sent.shape, sent.dtype),
        scratch_shapes=[
            pltpu.VMEM((groups, 2) + block[1:], sent.dtype),
            pltpu.VMEM(gate_half.shape, gate_half.dtype),
            pltpu.VMEM(up_half.shape, up_half.dtype),
            pltpu.VMEM(down_half.shape, down_half.dtype),
            pltpu.VMEM(block[1:], sent.dtype),
            pltpu.VMEM(block, sent.dtype),
            pltpu.VMEM(block, sent.dtype),
            pltpu.VMEM(block, sent.dtype),
            each,
            each,
            few,
            few,
            few,
            few,
            each,
            each,
            pltpu.SemaphoreType.DMA((4,)),
        ],
        compiler_params=pltpu.CompilerParams(collective_id=1, has_side_effects=True),
        name="expert_exchange",
    )(sent, gate_half, up_half, down_half)


def per_device(
    query_matrix,
    key_matrix,
    value_matrix,
    output_gate_logits,
    decay_preactivation,
    head_extra_decay,
    residual,
    head_norm_gain,
    output_projection_weight,
    mixer_norm_gain,
    routes,
    routing_weight,
    routed_gate_weight,
    routed_up_weight,
    routed_down_weight,
    common_gate_weight,
    common_up_weight,
    common_down_weight,
    final_norm_gain,
):
    local_out, wide, state, total = local_part(
        query_matrix, key_matrix, value_matrix, decay_preactivation, head_extra_decay
    )
    entered = exchange(state, total)
    gain = jnp.concatenate([head_norm_gain] * (LANES // KEY_HEAD_SIZE))[None]
    gated = finish_part(local_out, wide, entered, output_gate_logits, gain)
    projected = lax.psum_scatter(
        jnp.dot(gated, output_projection_weight, preferred_element_type=jnp.float32).astype(
            jnp.bfloat16
        ),
        "tp",
        scatter_dimension=0,
        tiled=True,
    ).astype(jnp.float32)
    normed = layer_norm(residual.astype(jnp.float32) + projected, mixer_norm_gain).astype(
        jnp.bfloat16
    )
    row_count = normed.shape[0]
    model_width = normed.shape[1]
    top_count = routes.shape[1]
    experts = lax.axis_size("sp")
    capacity = max(2, row_count * top_count // experts * 2)
    flat_expert = routes.reshape(-1)
    member = (flat_expert[:, None] == jnp.arange(experts, dtype=jnp.int32)[None, :]).astype(
        jnp.int32
    )
    rank_in = jnp.sum((jnp.cumsum(member, axis=0) - member) * member, axis=1)
    slot_of = flat_expert * capacity + rank_in
    source_row = (
        jnp.zeros((experts * capacity,), jnp.int32)
        .at[slot_of]
        .set(jnp.arange(row_count * top_count, dtype=jnp.int32) // top_count)
    )
    outbound = normed[source_row].reshape(experts, capacity, model_width)
    gate_half = routed_gate_weight[0]
    up_half = routed_up_weight[0]
    down_half = routed_down_weight[0]
    expert_out = expert_exchange(outbound, gate_half, up_half, down_half)
    flat_out = expert_out.reshape(experts * capacity, model_width)
    picked = flat_out[slot_of].astype(jnp.float32).reshape(row_count, top_count, model_width)
    routed = jnp.einsum("rk,rkd->rd", routing_weight, picked)
    shared_gate_out = jnp.dot(normed, common_gate_weight, preferred_element_type=jnp.float32)
    shared_up_out = jnp.dot(normed, common_up_weight, preferred_element_type=jnp.float32)
    shared_inner = (jax.nn.silu(shared_gate_out) * shared_up_out).astype(jnp.bfloat16)
    feed = jnp.dot(shared_inner, common_down_weight, preferred_element_type=jnp.float32) + routed
    return layer_norm(normed.astype(jnp.float32) + feed, final_norm_gain).astype(jnp.bfloat16)


def solution(mesh):
    placed = (
        P("sp", "tp"),
        P("sp", "tp"),
        P("sp", "tp"),
        P("sp", "tp"),
        P("sp", "tp"),
        P("sp", "tp"),
        P(("sp", "tp"), None),
        P(),
        P("tp", None),
        P(),
        P(("sp", "tp"), None),
        P(("sp", "tp"), None),
        P("sp", None, "tp"),
        P("sp", None, "tp"),
        P("sp", "tp", None),
        P(),
        P(),
        P(),
        P(),
    )
    return jax.shard_map(
        per_device, mesh=mesh, in_specs=placed, out_specs=P(("sp", "tp"), None), check_vma=False
    )
```
